32 devices in a mesh: ep: 8 (over z, x), tp: 4 (over y, core).
Axes of the slice: x: 2, y: 2, z: 4, core: 2. Of those that a mesh axis runs over, the one named last changes fastest.
Arguments:
- tokens: bfloat16 [1024, 2048], P('ep'), may hold values from -6 to 6
- norm_gain: float32 [2048], replicated, may hold values from 0.1 to 1.9
- expert_ids: int32 [1024, 2], P('ep'), may hold values from 0 to 7, all different within a row; in each aligned block of 128 rows (0 to 127, 128 to 255, ...) at most 64 rows name the same one
- route_weights: float32 [1024, 2], P('ep'), may hold values from 0.2 to 1
- w_gate: bfloat16 [8, 2048, 4096], P('ep', None, 'tp'), may hold values from -0.125 to 0.125
- w_up: bfloat16 [8, 2048, 4096], P('ep', None, 'tp'), may hold values from -0.125 to 0.125
- w_down: bfloat16 [8, 4096, 2048], P('ep', 'tp'), may hold values from -0.09375 to 0.09375
Outputs:
- combined: bfloat16 [1024, 2048], P('ep', 'tp')
The draws below stay inside these ranges and needn't reach their ends.
Inputs may be any that keep to these rules, and one draw needn't show every extreme that they name: `expert_ids`: each row names two different experts; among the rows of one device no expert is named more than 64 times, and in every draw some expert is named exactly 64 times there.
All inputs are finite; a program needn't handle non-finite values.
Results may differ from the reference program's by a relative error of at most 0.019.
Values may be sent and summed in bfloat16 or wider, within the bound.
No kernel may reach another device: no remote copies, remote signals or barrier semaphores. Data moves between devices by JAX's collectives and lax.ppermute only.
A program may use at most 64 MiB of HBM per device.

```python
import math
import jax
import jax.numpy as jnp
import numpy as np
from jax import lax

D = 2048
FF = 4096
TOK_DEV = 128
EXPERTS = 8
CAP = 64
TOKENS = 1024
N_EP = 8
N_TP = 4


def block_scale(own_key, extent, pieces, low, top_value):
    loudness = 1.0
    for axis_at, blocks in pieces:
        draws = jax.random.uniform(jax.random.fold_in(jax.random.fold_in(own_key, 6), axis_at), (blocks,), jnp.float32, low / len(pieces), top_value / len(pieces))
        loudness = loudness * jnp.repeat(jnp.exp(draws), extent[axis_at] // blocks).reshape((-1,) + (1,) * (len(extent) - 1 - axis_at))
    return loudness


def routed_block(own_key, own, number, rows, count, top, bound, lean):
    sequence = jax.random.permutation(own_key, count)
    heavy_load, ordinary = shares(count, rows * top, bound, lean, True), shares(count, rows * top, bound, lean, False)
    places = jnp.arange(count)

    def named(sizes, turn):
        used = int((sizes > 0).sum())
        fixed = max(1, used // 4)
        passed = fixed + (places - fixed + turn * (used - fixed)) % max(1, count - fixed)
        return jnp.zeros((count,), jnp.int32).at[sequence[jnp.where(places < fixed, places, passed)]].set(jnp.asarray(sizes, jnp.int32))

    sizes = jnp.where(number % 4 == 0, named(heavy_load, number // 4), named(ordinary, number - number // 4 - 1))
    mixed = jax.random.permutation(jax.random.fold_in(own, 3), count)
    giver, sink = mixed[0:count // 2 * 2:2], mixed[1:count // 2 * 2:2]
    margin = jnp.minimum(sizes[giver] - 1, bound - sizes[sink]) // 2
    margin = jnp.where((giver == sequence[0]) | (sink == sequence[0]) | (sizes[sink] == 0), 0, jnp.maximum(margin, 0))
    passed = jax.random.randint(jax.random.fold_in(own, 4), (count // 2,), 0, 1 << 20) % (margin + 1)
    sizes = sizes.at[giver].add(-passed).at[sink].add(passed)
    items = jnp.searchsorted(jnp.cumsum(sizes), jnp.arange(rows * top), side="right").astype(jnp.int32)
    listing = items.reshape(top, rows).T
    listing = listing[jax.random.permutation(jax.random.fold_in(own, 1), rows)]
    turn = jax.random.randint(jax.random.fold_in(own, 2), (rows, 1), 0, top)
    return jnp.take_along_axis(listing, (jnp.arange(top)[None, :] + turn) % top, axis=1)


def shares(count, total, reach, slope, full):
    portions = [(1 << 20) // math.isqrt(rank ** slope) + 1 for rank in range(1, count + 1)]
    largest = reach if full else min(reach, max(-(-total // count), total * portions[0] // sum(portions)))
    least = 1 if total - largest >= count - 1 else 0
    counts, spare = [largest] + [least] * (count - 1), total - largest - least * (count - 1)
    while spare > 0:
        candidates = [i for i in range(1, count) if counts[i] < largest] or [i for i in range(1, count) if counts[i] < reach]
        mass, budget = sum([portions[i] for i in candidates]), spare
        for i in candidates:
            more = min(reach - counts[i], max(1, budget * portions[i] // mass), spare)
            counts[i] = counts[i] + more
            spare = spare - more
    return np.array(counts)


def centred(stream_key, extent, width, limit, shards=(), kind=jnp.bfloat16):
    result = width * jax.random.normal(stream_key, extent, jnp.float32)
    if shards:
        result = result * block_scale(stream_key, extent, shards, -0.22, 0.18)
    return jnp.clip(result, -limit, limit).astype(kind)


def setup_inputs(seed: int = 0) -> dict:
    seeds = jax.random.split(jax.random.key(seed), 8)
    tokens = centred(seeds[0], (TOKENS, D), 1.0, 6.0, ((0, 8),))
    norm_gain = jnp.clip(1.0 + 0.18 * jax.random.normal(seeds[1], (D,), jnp.float32), 0.1, 1.9)
    expert_ids_keys = jax.random.split(jax.random.fold_in(seeds[2], 1), TOKENS // TOK_DEV)
    expert_ids_turns = jax.random.permutation(jax.random.fold_in(seeds[2], 3), TOKENS // TOK_DEV)
    expert_ids = jax.vmap(lambda own, number: routed_block(jax.random.fold_in(seeds[2], 2), own, number, TOK_DEV, EXPERTS, 2, CAP, 2))(expert_ids_keys, expert_ids_turns).reshape((TOKENS, 2))
    route_weights = jnp.clip(0.2 + 0.8 * jax.random.uniform(seeds[3], (TOKENS, 2), jnp.float32) ** block_scale(seeds[3], (TOKENS, 2), ((0, 8),), -0.2, 0.2), 0.2, 1.0)
    w_gate = centred(seeds[4], (EXPERTS, D, FF), D ** -0.5, 0.125, ((0, 8), (2, 4)))
    w_up = centred(seeds[5], (EXPERTS, D, FF), D ** -0.5, 0.125, ((0, 8), (2, 4)))
    w_down = centred(seeds[6], (EXPERTS, FF, D), FF ** -0.5, 0.09375, ((0, 8), (1, 4)))
    return {"tokens": tokens, "norm_gain": norm_gain, "expert_ids": expert_ids, "route_weights": route_weights, "w_gate": w_gate, "w_up": w_up, "w_down": w_down}


epsilon = 1e-06

def run_expert(operands):
    rows, gate_weight, up_weight, down_weight = operands
    model_width = rows.shape[1]
    gate_values = jnp.dot(rows, gate_weight, preferred_element_type=jnp.float32)
    up_values = jnp.dot(rows, up_weight, preferred_element_type=jnp.float32)
    hidden = (jax.nn.silu(gate_values) * up_values).astype(jnp.bfloat16)
    grouped = hidden.reshape(rows.shape[0], N_TP, -1).astype(jnp.float32)
    down_groups = down_weight.reshape(N_TP, -1, model_width).astype(jnp.float32)
    partial_value = jnp.einsum('rtf,tfd->trd', grouped, down_groups)
    partial_value = lax.optimization_barrier(partial_value.astype(jnp.bfloat16)).astype(jnp.float32)
    return lax.optimization_barrier(jnp.sum(partial_value, axis=0)).astype(jnp.bfloat16)

def reference(tokens, norm_gain, expert_ids, route_weights, w_gate, w_up, w_down):
    model_width = tokens.shape[1]
    as_float = tokens.astype(jnp.float32)
    scale = lax.rsqrt(lax.optimization_barrier(jnp.mean(as_float * as_float, axis=-1, keepdims=True)) + epsilon)
    normed = (as_float * scale * norm_gain[None, :]).astype(jnp.bfloat16)
    flat_ids = expert_ids.reshape(N_EP, TOK_DEV * 2).astype(jnp.int32)
    one_hot = (flat_ids[:, :, None] == jnp.arange(EXPERTS, dtype=jnp.int32)[None, None, :]).astype(jnp.int32)
    slot_index = lax.optimization_barrier(jnp.sum((jnp.cumsum(one_hot, axis=1) - one_hot) * one_hot, axis=-1)).astype(jnp.int32)
    source = jnp.arange(N_EP, dtype=jnp.int32)[:, None]
    target = (flat_ids * (N_EP * CAP) + source * CAP + slot_index).reshape(-1).astype(jnp.int32)
    token_rows = jnp.repeat(normed, 2, axis=0)
    buffer = jnp.zeros((EXPERTS * N_EP * CAP, model_width), jnp.bfloat16).at[target].set(token_rows)
    buffer = buffer.reshape(EXPERTS, N_EP * CAP, model_width)
    expert_out = lax.map(run_expert, (buffer, w_gate, w_up, w_down))
    picked = expert_out.reshape(-1, model_width)[target].reshape(TOKENS, 2, model_width).astype(jnp.float32)
    return lax.optimization_barrier(jnp.sum(picked * route_weights[:, :, None], axis=1)).astype(jnp.bfloat16)
```

```python
import functools

import jax
import jax.numpy as jnp
from jax import lax
from jax.experimental import pallas as pl
from jax.experimental.pallas import tpu as pltpu
from jax.sharding import PartitionSpec as P

epsilon = 1e-06


def plain_per_device(tokens, norm_gain, expert_ids, route_weights, w_gate, w_up, w_down):
    tok_rows, model_width = tokens.shape
    experts = w_gate.shape[0] * lax.axis_size("ep")
    column_width = model_width // lax.axis_size("tp")
    capacity = 4 * tok_rows // experts
    as_float = tokens.astype(jnp.float32)
    scale = lax.rsqrt(jnp.mean(as_float * as_float, axis=-1, keepdims=True) + epsilon)
    normed = (as_float * scale * norm_gain[None, :]).astype(jnp.bfloat16)
    flat_ids = expert_ids.reshape(-1)
    one_hot = (flat_ids[:, None] == jnp.arange(experts, dtype=jnp.int32)[None, :]).astype(jnp.int32)
    slot_index = jnp.sum((jnp.cumsum(one_hot, axis=0) - one_hot) * one_hot, axis=1)
    target = flat_ids * capacity + slot_index
    token_rows = jnp.repeat(normed, 2, axis=0)
    token_rows = lax.dynamic_slice_in_dim(
        token_rows, lax.axis_index("tp") * column_width, column_width, 1
    )
    outgoing = (
        jnp.zeros((experts * capacity, token_rows.shape[1]), jnp.bfloat16)
        .at[target]
        .set(token_rows)
    )
    outgoing = outgoing.reshape(experts, capacity, token_rows.shape[1])
    arrived = lax.all_to_all(outgoing, "ep", split_axis=0, concat_axis=1, tiled=True)
    piece = lax.all_gather(arrived, "tp", axis=2, tiled=True)
    gate_part = jnp.einsum("erd,edf->erf", piece, w_gate, preferred_element_type=jnp.float32)
    up_part = jnp.einsum("erd,edf->erf", piece, w_up, preferred_element_type=jnp.float32)
    hidden = (jax.nn.silu(gate_part) * up_part).astype(jnp.bfloat16)
    partial_value = jnp.einsum("erf,efd->erd", hidden, w_down, preferred_element_type=jnp.float32)
    summed = lax.psum_scatter(
        partial_value.astype(jnp.bfloat16), "tp", scatter_dimension=2, tiled=True
    )
    returned = lax.all_to_all(summed, "ep", split_axis=1, concat_axis=0, tiled=True)
    picked = returned.reshape(experts * capacity, column_width)[target]
    picked = picked.reshape(tok_rows, 2, column_width).astype(jnp.float32)
    return jnp.sum(picked * route_weights[:, :, None], axis=1).astype(jnp.bfloat16)


def names_of(ids, lanes):
    lane = lax.broadcasted_iota(jnp.int32, (ids.shape[0], lanes), 1)
    return (ids[:, 0:1] == lane) | (ids[:, 1:2] == lane)


def pack_kernel(place, tokens, gain, ids, *rest, experts, capacity, width):
    outs, (slots,) = rest[:experts], rest[experts:]
    rows = tokens.shape[0]
    as_float = tokens[...].astype(jnp.float32)
    scale = lax.rsqrt(jnp.mean(as_float * as_float, axis=-1, keepdims=True) + epsilon)
    start = pl.multiple_of(place[1] * width, width)
    own = tokens[:, pl.ds(start, width)].astype(jnp.float32)
    normed = (own * scale * gain[:, pl.ds(start, width)]).astype(jnp.bfloat16)
    named = names_of(ids[...], 128).astype(jnp.float32).astype(jnp.bfloat16)
    before = lax.broadcasted_iota(jnp.int32, (rows, rows), 0)
    after = lax.broadcasted_iota(jnp.int32, (rows, rows), 1)
    to_bf = lambda m: m.astype(jnp.float32).astype(jnp.bfloat16)
    turned = lambda m: lax.dot_general(
        named, to_bf(m), (((0,), (0,)), ((), ())), preferred_element_type=jnp.float32
    )
    slots[...] = jnp.where(turned(before == after) > 0.5, turned(before < after), -1.0)
    place_in = lax.broadcasted_iota(jnp.int32, (capacity, rows), 0).astype(jnp.float32)
    for k in range(experts):
        line = slots[pl.ds(place[0] ^ k, 1), :]
        chosen = to_bf(line == place_in)
        outs[k][...] = jnp.dot(chosen, normed, preferred_element_type=jnp.float32).astype(
            jnp.bfloat16
        )


def merge_kernel(place, ids, weights, *rest, capacity):
    arrived, out = rest[:-1], rest[-1]
    rows = ids.shape[0]
    pair = ids[...]
    named = names_of(pair, 128)
    before = lax.broadcasted_iota(jnp.int32, (rows, rows), 0)
    after = lax.broadcasted_iota(jnp.int32, (rows, rows), 1)
    to_bf = lambda m: m.astype(jnp.float32).astype(jnp.bfloat16)
    slot = jnp.dot(to_bf(after < before), to_bf(named), preferred_element_type=jnp.float32)
    lane = lax.broadcasted_iota(jnp.int32, (rows, 128), 1)
    slot_lane = lax.broadcasted_iota(jnp.int32, (rows, capacity), 1).astype(jnp.float32)
    total = None
    for k, ref in enumerate(arrived):
        expert = place[0] ^ k
        column = jnp.sum(jnp.where((lane == expert) & named, slot + 1.0, 0.0), axis=1, keepdims=True)
        chosen = to_bf(column - 1.0 == slot_lane)
        weight = jnp.sum(jnp.where(pair == expert, weights[...], 0.0), axis=1, keepdims=True)
        term = weight * jnp.dot(chosen, ref[...], preferred_element_type=jnp.float32)
        total = term if total is None else total + term
    out[...] = total.astype(jnp.bfloat16)


def ffn_kernel(place, w_gate, w_up, w_down, *rest, groups, ranks, chunks):
    pieces = rest[: groups * ranks]
    outs = rest[groups * ranks : 2 * groups * ranks]
    x, gate, up, down, hidden, sems = rest[2 * groups * ranks :]
    width = pieces[0].shape[1]
    rows = pieces[0].shape[0]
    step = gate.shape[1] // chunks
    copies = []
    for j in range(chunks):
        part = pl.ds(j * step, step)
        copies.append(
            (
                pltpu.make_async_copy(w_gate.at[0, :, part], gate.at[:, part], sems.at[0, j]),
                pltpu.make_async_copy(w_up.at[0, :, part], up.at[:, part], sems.at[1, j]),
            )
        )
    last = [
        pltpu.make_async_copy(
            w_down.at[0, pl.ds(j * step, step)], down.at[pl.ds(j * step, step)], sems.at[2, j]
        )
        for j in range(chunks)
    ]
    for pair in copies:
        for copy in pair:
            copy.start()
    for copy in last:
        copy.start()
    for r in range(ranks):
        start = pl.multiple_of((place[1] ^ r) * width, width)
        for g in range(groups):
            x[g * rows : (g + 1) * rows, pl.ds(start, width)] = pieces[g * ranks + r][...]
    for j in range(chunks):
        part = slice(j * step, (j + 1) * step)
        for copy in copies[j]:
            copy.wait()
        g_value = jnp.dot(x[...], gate[:, part], preferred_element_type=jnp.float32)
        u_value = jnp.dot(x[...], up[:, part], preferred_element_type=jnp.float32)
        hidden[:, part] = (g_value / (1.0 + jnp.exp(-g_value)) * u_value).astype(jnp.bfloat16)
    for copy in last:
        copy.wait()
    for r in range(ranks):
        start = pl.multiple_of((place[1] ^ r) * width, width)
        value = jnp.dot(
            hidden[...], down[:, pl.ds(start, width)], preferred_element_type=jnp.float32
        ).astype(jnp.bfloat16)
        for g in range(groups):
            outs[g * ranks + r][...] = value[g * rows : (g + 1) * rows]


def swap(value, axis, mask):
    size = lax.axis_size(axis)
    return lax.ppermute(value, axis, [(i, i ^ mask) for i in range(size)])


def per_device(tokens, norm_gain, expert_ids, route_weights, w_gate, w_up, w_down):
    rows, model_width = tokens.shape
    peers, ranks = lax.axis_size("ep"), lax.axis_size("tp")
    width = model_width // ranks
    capacity = 4 * rows // peers
    units = w_gate.shape[2]
    place = jnp.stack([lax.axis_index("ep"), lax.axis_index("tp")]).astype(jnp.int32)
    smem = pl.BlockSpec(memory_space=pltpu.SMEM)
    vmem = pl.BlockSpec(memory_space=pltpu.VMEM)
    hbm = pl.BlockSpec(memory_space=pl.ANY)
    block = jax.ShapeDtypeStruct((capacity, width), jnp.bfloat16)
    sent = pl.pallas_call(
        functools.partial(pack_kernel, experts=peers, capacity=capacity, width=width),
        out_shape=[block] * peers,
        in_specs=[smem, vmem, vmem, vmem],
        out_specs=[vmem] * peers,
        scratch_shapes=[pltpu.VMEM((128, rows), jnp.float32)],
        name="pack",
    )(place, tokens, norm_gain.reshape(1, -1), expert_ids)
    order = sorted(range(1, peers), reverse=True)
    got = {0: sent[0]}
    for k in order:
        got[k] = swap(sent[k], "ep", k)
    groups = peers // 2
    pieces = {}
    for g in sorted(range(groups), reverse=True):
        mine = jnp.concatenate([got[2 * g], got[2 * g + 1]], axis=0)
        other = swap(mine, "tp", 2)
        pieces[g] = [mine, swap(mine, "tp", 1), other, swap(other, "tp", 1)]
    flat = [pieces[g][r] for g in range(groups) for r in range(ranks)]
    pair_block = jax.ShapeDtypeStruct((2 * capacity, width), jnp.bfloat16)
    chunks = 4
    parts = pl.pallas_call(
        functools.partial(ffn_kernel, groups=groups, ranks=ranks, chunks=chunks),
        out_shape=[pair_block] * (groups * ranks),
        in_specs=[smem, hbm, hbm, hbm] + [vmem] * (groups * ranks),
        out_specs=[vmem] * (groups * ranks),
        scratch_shapes=[
            pltpu.VMEM((peers * capacity, model_width), jnp.bfloat16),
            pltpu.VMEM((model_width, units), jnp.bfloat16),
            pltpu.VMEM((model_width, units), jnp.bfloat16),
            pltpu.VMEM((units, model_width), jnp.bfloat16),
            pltpu.VMEM((peers * capacity, units), jnp.bfloat16),
            pltpu.SemaphoreType.DMA((3, chunks)),
        ],
        name="ffn",
    )(place, w_gate, w_up, w_down, *flat)
    f32 = lambda v: v.astype(jnp.float32)
    home = {}
    for g in sorted(range(groups), reverse=True):
        own = parts[g * ranks : (g + 1) * ranks]
        far = (f32(own[2]) + f32(swap(own[3], "tp", 1))).astype(jnp.bfloat16)
        near = f32(own[0]) + f32(swap(own[1], "tp", 1))
        total = (near + f32(swap(far, "tp", 2))).astype(jnp.bfloat16)
        for half in (1, 0):
            k = 2 * g + half
            piece = total[half * capacity : (half + 1) * capacity]
            home[k] = swap(piece, "ep", k) if k else piece
    return pl.pallas_call(
        functools.partial(merge_kernel, capacity=capacity),
        out_shape=jax.ShapeDtypeStruct((rows, width), jnp.bfloat16),
        in_specs=[smem, vmem, vmem] + [vmem] * peers,
        out_specs=vmem,
        name="merge",
    )(place, expert_ids, route_weights, *[home[k] for k in range(peers)])


def solution(mesh):
    in_specs = (
        P("ep", None),
        P(),
        P("ep", None),
        P("ep", None),
        P("ep", None, "tp"),
        P("ep", None, "tp"),
        P("ep", "tp", None),
    )
    out_specs = P("ep", "tp")
    peers, ranks = mesh.shape["ep"], mesh.shape["tp"]

    def body(*arrays):
        tokens, w_gate = arrays[0], arrays[4]
        capacity = 4 * tokens.shape[0] // (peers * w_gate.shape[0])
        paired = (
            ranks == 4
            and 2 <= peers <= 16
            and peers & (peers - 1) == 0
            and w_gate.shape[0] == 1
            and tokens.shape[0] == 128
            and capacity % 16 == 0
            and tokens.shape[1] % (128 * ranks) == 0
            and w_gate.shape[2] % 512 == 0
        )
        return (per_device if paired else plain_per_device)(*arrays)

    return jax.shard_map(
        body, mesh=mesh, in_specs=in_specs, out_specs=out_specs, check_vma=False
    )
```

```python
import functools

import jax
import jax.numpy as jnp
from jax import lax
from jax.experimental import pallas as pl
from jax.experimental.pallas import tpu as pltpu
from jax.sharding import PartitionSpec as P

epsilon = 1e-06


def plain_per_device(tokens, norm_gain, expert_ids, route_weights, w_gate, w_up, w_down):
    tok_rows, model_width = tokens.shape
    experts = w_gate.shape[0] * lax.axis_size("ep")
    column_width = model_width // lax.axis_size("tp")
    capacity = 4 * tok_rows // experts
    as_float = tokens.astype(jnp.float32)
    scale = lax.rsqrt(jnp.mean(as_float * as_float, axis=-1, keepdims=True) + epsilon)
    normed = (as_float * scale * norm_gain[None, :]).astype(jnp.bfloat16)
    flat_ids = expert_ids.reshape(-1)
    one_hot = (flat_ids[:, None] == jnp.arange(experts, dtype=jnp.int32)[None, :]).astype(jnp.int32)
    slot_index = jnp.sum((jnp.cumsum(one_hot, axis=0) - one_hot) * one_hot, axis=1)
    target = flat_ids * capacity + slot_index
    token_rows = jnp.repeat(normed, 2, axis=0)
    token_rows = lax.dynamic_slice_in_dim(
        token_rows, lax.axis_index("tp") * column_width, column_width, 1
    )
    outgoing = (
        jnp.zeros((experts * capacity, token_rows.shape[1]), jnp.bfloat16)
        .at[target]
        .set(token_rows)
    )
    outgoing = outgoing.reshape(experts, capacity, token_rows.shape[1])
    arrived = lax.all_to_all(outgoing, "ep", split_axis=0, concat_axis=1, tiled=True)
    piece = lax.all_gather(arrived, "tp", axis=2, tiled=True)
    gate_part = jnp.einsum("erd,edf->erf", piece, w_gate, preferred_element_type=jnp.float32)
    up_part = jnp.einsum("erd,edf->erf", piece, w_up, preferred_element_type=jnp.float32)
    hidden = (jax.nn.silu(gate_part) * up_part).astype(jnp.bfloat16)
    partial_value = jnp.einsum("erf,efd->erd", hidden, w_down, preferred_element_type=jnp.float32)
    summed = lax.psum_scatter(
        partial_value.astype(jnp.bfloat16), "tp", scatter_dimension=2, tiled=True
    )
    returned = lax.all_to_all(summed, "ep", split_axis=1, concat_axis=0, tiled=True)
    picked = returned.reshape(experts * capacity, column_width)[target]
    picked = picked.reshape(tok_rows, 2, column_width).astype(jnp.float32)
    return jnp.sum(picked * route_weights[:, :, None], axis=1).astype(jnp.bfloat16)


def eye(rows):
    return lax.broadcasted_iota(jnp.int32, (rows, rows), 0) == lax.broadcasted_iota(
        jnp.int32, (rows, rows), 1
    )


def to_bf(mask):
    return mask.astype(jnp.float32).astype(jnp.bfloat16)


def pack_kernel(tokens, gain, ids, *rest, experts, capacity, width):
    outs, (slots,) = rest[:-1], rest[-1:]
    rows = tokens.shape[0]
    me = lax.axis_index("ep")
    as_float = tokens[...].astype(jnp.float32)
    scale = lax.rsqrt(jnp.mean(as_float * as_float, axis=-1, keepdims=True) + epsilon)
    start = pl.multiple_of(lax.axis_index("tp") * width, width)
    own = tokens[:, pl.ds(start, width)].astype(jnp.float32)
    normed = (own * scale * gain[:, pl.ds(start, width)]).astype(jnp.bfloat16)
    sub = lax.broadcasted_iota(jnp.int32, (16, rows), 0)
    named = (ids[0:1, :] == sub) | (ids[1:2, :] == sub)
    before = lax.broadcasted_iota(jnp.int32, (rows, rows), 0)
    after = lax.broadcasted_iota(jnp.int32, (rows, rows), 1)
    count = jnp.dot(to_bf(named), to_bf(before < after), preferred_element_type=jnp.float32)
    slots[...] = jnp.where(named, count, -1.0)
    place_in = lax.broadcasted_iota(jnp.int32, (capacity, rows), 0).astype(jnp.float32)
    for k in range(experts):
        chosen = to_bf(slots[pl.ds(me ^ k, 1), :] == place_in)
        outs[k][...] = jnp.dot(chosen, normed, preferred_element_type=jnp.float32).astype(
            jnp.bfloat16
        )


def merge_kernel(ids, weights, *rest, capacity):
    arrived, out = rest[:-1], rest[-1]
    rows = ids.shape[1]
    me = lax.axis_index("ep")
    diagonal = eye(rows)
    column = lambda line, zero: jnp.sum(jnp.where(diagonal, line, zero), axis=1, keepdims=True)
    first, second = (column(ids[i : i + 1, :].astype(jnp.float32), 0.0) for i in (0, 1))
    first_weight, second_weight = (column(weights[i : i + 1, :], 0.0) for i in (0, 1))
    lane = lax.broadcasted_iota(jnp.int32, (rows, 128), 1)
    lane_float = lane.astype(jnp.float32)
    named = (first == lane_float) | (second == lane_float)
    before = lax.broadcasted_iota(jnp.int32, (rows, rows), 0)
    after = lax.broadcasted_iota(jnp.int32, (rows, rows), 1)
    slot = jnp.dot(to_bf(after < before), to_bf(named), preferred_element_type=jnp.float32)
    slot_lane = lax.broadcasted_iota(jnp.int32, (rows, capacity), 1).astype(jnp.float32)
    total = None
    for k, ref in enumerate(arrived):
        expert = me ^ k
        which = expert.astype(jnp.float32)
        position = jnp.sum(
            jnp.where((lane == expert) & named, slot + 1.0, 0.0), axis=1, keepdims=True
        )
        chosen = to_bf(position - 1.0 == slot_lane)
        weight = jnp.where(first == which, first_weight, 0.0)
        weight = jnp.where(second == which, second_weight, weight)
        term = weight * jnp.dot(chosen, ref[...], preferred_element_type=jnp.float32)
        total = term if total is None else total + term
    out[...] = total.astype(jnp.bfloat16)


def ffn_kernel(w_gate, w_up, w_down, *rest, groups, ranks, chunks):
    count = groups * ranks
    pieces = rest[:count]
    near = rest[count : count + 2 * groups]
    far = rest[count + 2 * groups : count + 2 * groups + 2]
    x, landed, gate, up, down, hidden, x_sems, w_sems = rest[count + 2 * groups + 2 :]
    me = lax.axis_index("tp")
    rows, width = pieces[0].shape
    step = gate.shape[1] // chunks
    places = [pl.ds(pl.multiple_of((me ^ r) * width, width), width) for r in range(ranks)]
    loads = [
        pltpu.make_async_copy(pieces[i], landed.at[i], x_sems.at[i]) for i in range(count)
    ]
    weights, last = [], []
    for j in range(chunks):
        part = pl.ds(j * step, step)
        weights.append(
            (
                pltpu.make_async_copy(w_gate.at[0, :, part], gate.at[:, part], w_sems.at[0, j]),
                pltpu.make_async_copy(w_up.at[0, :, part], up.at[:, part], w_sems.at[1, j]),
            )
        )
        last.append(pltpu.make_async_copy(w_down.at[0, part], down.at[part], w_sems.at[2, j]))
    for copy in loads:
        copy.start()
    for pair in weights:
        for copy in pair:
            copy.start()
    for copy in last:
        copy.start()
    for copy in loads:
        copy.wait()
    for r in range(ranks):
        for g in range(groups):
            x[g * rows : (g + 1) * rows, places[r]] = landed[g * ranks + r]
    for j in range(chunks):
        part = slice(j * step, (j + 1) * step)
        for copy in weights[j]:
            copy.wait()
        g_value = jnp.dot(x[...], gate[:, part], preferred_element_type=jnp.float32)
        u_value = jnp.dot(x[...], up[:, part], preferred_element_type=jnp.float32)
        hidden[:, part] = (g_value / (1.0 + jnp.exp(-g_value)) * u_value).astype(jnp.bfloat16)
    for copy in last:
        copy.wait()
    for r in range(ranks):
        value = jnp.dot(hidden[...], down[:, places[r]], preferred_element_type=jnp.float32)
        value = value.astype(jnp.bfloat16)
        if r >= 2:
            far[r - 2][...] = value
        else:
            for g in range(groups):
                near[2 * g + r][...] = value[g * rows : (g + 1) * rows]


def swap(value, axis, mask):
    size = lax.axis_size(axis)
    return lax.ppermute(value, axis, [(i, i ^ mask) for i in range(size)])


def paired_device(tokens, norm_gain, expert_ids, route_weights, w_gate, w_up, w_down):
    rows, model_width = tokens.shape
    peers, ranks = lax.axis_size("ep"), lax.axis_size("tp")
    width = model_width // ranks
    capacity = 4 * rows // peers
    units = w_gate.shape[2]
    vmem = pl.BlockSpec(memory_space=pltpu.VMEM)
    block = jax.ShapeDtypeStruct((capacity, width), jnp.bfloat16)
    sent = pl.pallas_call(
        functools.partial(pack_kernel, experts=peers, capacity=capacity, width=width),
        out_shape=[block] * peers,
        in_specs=[vmem] * 3,
        out_specs=[vmem] * peers,
        scratch_shapes=[pltpu.VMEM((16, rows), jnp.float32)],
        name="pack",
    )(tokens, norm_gain.reshape(1, -1), expert_ids.T)
    got = {0: sent[0]}
    for k in reversed(range(1, peers)):
        got[k] = swap(sent[k], "ep", k)
    groups = peers // 2
    pieces = {}
    for g in reversed(range(groups)):
        mine = jnp.concatenate([got[2 * g], got[2 * g + 1]], axis=0)
        other = swap(mine, "tp", 2)
        pieces[g] = [mine, swap(mine, "tp", 1), other, swap(other, "tp", 1)]
    flat = [pieces[g][r] for g in range(groups) for r in range(ranks)]
    slots = peers * capacity
    pair_block = jax.ShapeDtypeStruct((2 * capacity, width), jnp.bfloat16)
    whole = jax.ShapeDtypeStruct((slots, width), jnp.bfloat16)
    chunks = 4
    anywhere = pl.BlockSpec(memory_space=pl.ANY)
    parts = pl.pallas_call(
        functools.partial(ffn_kernel, groups=groups, ranks=ranks, chunks=chunks),
        out_shape=[pair_block] * (2 * groups) + [whole] * 2,
        in_specs=[anywhere] * (3 + groups * ranks),
        out_specs=[vmem] * (2 * groups + 2),
        scratch_shapes=[
            pltpu.VMEM((slots, model_width), jnp.bfloat16),
            pltpu.VMEM((groups * ranks, 2 * capacity, width), jnp.bfloat16),
            pltpu.VMEM((model_width, units), jnp.bfloat16),
            pltpu.VMEM((model_width, units), jnp.bfloat16),
            pltpu.VMEM((units, model_width), jnp.bfloat16),
            pltpu.VMEM((slots, units), jnp.bfloat16),
            pltpu.SemaphoreType.DMA((groups * ranks,)),
            pltpu.SemaphoreType.DMA((3, chunks)),
        ],
        name="ffn",
    )(w_gate, w_up, w_down, *flat)
    f32 = lambda v: v.astype(jnp.float32)
    far = (f32(parts[-2]) + f32(swap(parts[-1], "tp", 1))).astype(jnp.bfloat16)
    home = {}
    for g in reversed(range(groups)):
        crossed = swap(far[2 * g * capacity : 2 * (g + 1) * capacity], "tp", 2)
        near = f32(parts[2 * g]) + f32(swap(parts[2 * g + 1], "tp", 1))
        total = (near + f32(crossed)).astype(jnp.bfloat16)
        for half in (1, 0):
            k = 2 * g + half
            piece = total[half * capacity : (half + 1) * capacity]
            home[k] = swap(piece, "ep", k) if k else piece
    return pl.pallas_call(
        functools.partial(merge_kernel, capacity=capacity),
        out_shape=jax.ShapeDtypeStruct((rows, width), jnp.bfloat16),
        in_specs=[vmem] * (2 + peers),
        out_specs=vmem,
        name="merge",
    )(expert_ids.T, route_weights.T, *[home[k] for k in range(peers)])


def solution(mesh):
    in_specs = (
        P("ep", None),
        P(),
        P("ep", None),
        P("ep", None),
        P("ep", None, "tp"),
        P("ep", None, "tp"),
        P("ep", "tp", None),
    )
    out_specs = P("ep", "tp")
    peers, ranks = mesh.shape["ep"], mesh.shape["tp"]

    def body(*arrays):
        tokens, w_gate = arrays[0], arrays[4]
        capacity = 4 * tokens.shape[0] // (peers * w_gate.shape[0])
        paired = (
            ranks == 4
            and 2 <= peers <= 16
            and peers & (peers - 1) == 0
            and w_gate.shape[0] == 1
            and tokens.shape[0] == 128
            and capacity % 16 == 0
            and tokens.shape[1] % (128 * ranks) == 0
            and w_gate.shape[2] % 512 == 0
        )
        return (paired_device if paired else plain_per_device)(*arrays)

    return jax.shard_map(
        body, mesh=mesh, in_specs=in_specs, out_specs=out_specs, check_vma=False
    )
```
